32 devices in a mesh: grp: 2 (over x), tp: 4 (over z), dp: 4 (over y, core).
Axes of the slice: x: 2, y: 2, z: 4, core: 2. Of those that a mesh axis runs over, the one named last changes fastest.
Arguments:
- tokens: bfloat16 [32, 4096], P(('grp', 'tp'), 'dp'), parts along dimension 0, may hold values from -30 to 30
- norm_gain: float32 [2, 4096], P(None, 'dp'), may hold values from 0.1 to 1.9
- w_query: bfloat16 [2, 4096, 2048], P(None, 'dp', 'tp'), may hold values from -0.09375 to 0.09375
- w_forget: bfloat16 [2, 4096, 2048], P(None, 'dp', 'tp'), may hold values from -0.09375 to 0.09375
- w_value: bfloat16 [2, 4096, 2048], P(None, 'dp', 'tp'), may hold values from -0.09375 to 0.09375
- w_gate: bfloat16 [2, 4096, 2048], P(None, 'dp', 'tp'), may hold values from -0.09375 to 0.09375
- lower_bound: float32 [2, 2048], P(None, 'tp'), may hold values from 0 to 0.9
- head_gain: float32 [2, 128], replicated, may hold values from 0.1 to 1.9
- w_out: bfloat16 [2, 2048, 4096], P(None, 'tp', 'dp'), may hold values from -0.125 to 0.125
- state: float32 [2, 32, 16, 128, 128], P(None, ('grp', 'dp'), 'tp'), parts along dimension 1, may hold values from -4 to 4
Outputs:
- hidden_out: bfloat16 [32, 4096], P(('grp', 'tp'), 'dp'), parts along dimension 0
- new_state: float32 [2, 32, 16, 128, 128], P(None, ('grp', 'dp'), 'tp'), parts along dimension 1
The draws below stay inside these ranges and needn't reach their ends.
There are 2 independent parts, one for each index of `grp`. The reference program is written for one: setup_inputs(seed, part) draws one part's arguments, and reference() takes and returns one part's arrays. A program takes and returns all parts, laid end to end along the dimension named above; an argument that names none is the same for every part. Nothing has to cross between parts.
All inputs are finite; a program needn't handle non-finite values.
Results may differ from the reference program's by a relative error of at most 0.02.
Values may be sent and summed in bfloat16 or wider, within the bound.
A program may use at most 64 MiB of HBM per device.

```python
import jax
import jax.numpy as jnp
from jax import lax

D = 4096
HEADS = 16
HD = 128
DH = 2048
BATCH = 16


def draw_tokens(key, part):
    first_key, second_key = jax.random.split(key, 2)
    column_scale = jnp.repeat(jnp.exp(jax.random.uniform(second_key, (D // 16,), jnp.float32, -1.2, 1.2)), 16)
    values = jax.random.normal(first_key, (BATCH, D), jnp.float32) * column_scale
    return jnp.clip(values, -30.0, 30.0).astype(jnp.bfloat16)


def block_scale(own_key, extent, cuts, low, top_value):
    def one(position, blocks):
        steps = jax.random.uniform(jax.random.fold_in(jax.random.fold_in(own_key, 6), position), (blocks,), jnp.float32, low / len(cuts), top_value / len(cuts))
        return jnp.repeat(jnp.exp(steps), extent[position] // blocks).reshape((-1,) + (1,) * (len(extent) - position - 1))

    level = one(*cuts[0])
    for cut in cuts[1:]:
        level = level * one(*cut)
    return level


def centred(key, dims, width, most, cuts=(), dtype=jnp.bfloat16):
    level = block_scale(key, dims, cuts, -0.22, 0.18) if cuts else 1.0
    values = jax.random.normal(key, dims, jnp.float32) * width * level
    return jnp.minimum(jnp.maximum(values, -most), most).astype(dtype)


def setup_inputs(seed: int = 0, part: int = 0) -> dict:
    key_of = jax.random.split(jax.random.key(seed), 11)
    own_keys = jax.random.split(jax.random.fold_in(key_of[10], part), 11)
    return {
        "tokens": draw_tokens(jax.random.fold_in(jax.random.fold_in(key_of[10], part), 71), part),
        "norm_gain": jnp.clip(1.0 + 0.18 * jax.random.normal(key_of[1], (2, D), jnp.float32), 0.1, 1.9),
        "w_query": centred(key_of[2], (2, D, DH), D ** -0.5, 0.09375, ((1, 4), (2, 4))),
        "w_forget": centred(key_of[3], (2, D, DH), D ** -0.5, 0.09375, ((1, 4), (2, 4))),
        "w_value": centred(key_of[4], (2, D, DH), D ** -0.5, 0.09375, ((1, 4), (2, 4))),
        "w_gate": centred(key_of[5], (2, D, DH), D ** -0.5, 0.09375, ((1, 4), (2, 4))),
        "lower_bound": jnp.clip(0.9 * jax.random.uniform(key_of[6], (2, DH), jnp.float32) ** block_scale(key_of[6], (2, DH), ((1, 4),), -0.2, 0.2), 0.0, 0.9),
        "head_gain": jnp.clip(1.0 + 0.18 * jax.random.normal(key_of[7], (2, HD), jnp.float32), 0.1, 1.9),
        "w_out": centred(key_of[8], (2, DH, D), DH ** -0.5, 0.125, ((1, 4), (2, 4))),
        "state": centred(own_keys[9], (2, BATCH, HEADS, HD, HD), 0.5, 4.0, ((1, 4), (2, 4)), jnp.float32),
    }


def reference(tokens, norm_gain, w_query, w_forget, w_value, w_gate, lower_bound, head_gain, w_out, state):
    hidden = tokens
    updated = []
    for layer in range(2):
        widened = hidden.astype(jnp.float32)
        factor = lax.rsqrt(lax.optimization_barrier(jnp.mean(widened * widened, axis=1, keepdims=True)) + 1e-06)
        scaled = (widened * norm_gain[layer]).astype(jnp.bfloat16)
        query = jnp.dot(scaled, w_query[layer], preferred_element_type=jnp.float32) * factor
        forget_pre = jnp.dot(scaled, w_forget[layer], preferred_element_type=jnp.float32) * factor
        value = jnp.dot(scaled, w_value[layer], preferred_element_type=jnp.float32) * factor
        gate_pre = jnp.dot(scaled, w_gate[layer], preferred_element_type=jnp.float32) * factor
        bound = lower_bound[layer]
        forget = bound + (1.0 - bound) * jax.nn.sigmoid(forget_pre)
        keyvec = (1.0 - bound) * jax.nn.sigmoid(-forget_pre)
        count = hidden.shape[0]
        head_count = query.shape[1] // HD
        shaped = lambda arr: arr.reshape(count, head_count, HD)
        carried = shaped(forget)[..., None] * state[layer] + shaped(keyvec)[..., None] * shaped(value)[..., None, :]
        updated.append(carried)
        readout = jnp.einsum('bhkv,bhk->bhv', carried, shaped(query))
        readout = readout * lax.rsqrt(lax.optimization_barrier(jnp.mean(readout * readout, axis=-1, keepdims=True)) + 1e-06) * head_gain[layer]
        normed = (readout.reshape(count, head_count * HD) * jax.nn.sigmoid(gate_pre)).astype(jnp.bfloat16)
        mixed = jnp.dot(normed, w_out[layer], preferred_element_type=jnp.float32)
        hidden = (widened + mixed).astype(jnp.bfloat16)
    return (hidden, jnp.stack(updated))
```

```python
import functools

import jax
import jax.numpy as jnp
from jax import lax
from jax.experimental import pallas as pl
from jax.experimental.pallas import tpu as pltpu
from jax.sharding import PartitionSpec as P

MESH = pl.DeviceIdType.MESH
LANES = 128
F32 = jnp.float32
BF16 = jnp.bfloat16


def each(count, body):
    if count <= 8:
        for d in range(1, count):
            body(d)
    else:

        @pl.loop(1, count)
        def _(d):
            body(d)


def kernel(
    tp, dp,
    tok, gain, wq, wf, wv, wg, bound_ref, head_gain, wo, st,
    out, ns,
    w_v, wo_v, s_v, xg, hf, h3, sq2, sqs, sqr, pf, ps, pr, tr_a, tr_b, ro,
    na, nf, po, ar, rs, rr,
    w_sem, wo_sem, s_sem, o_sem, xg_s, xg_r, sq_s, sq_r, p_s, p_r, n_s, n_r,
    ar_s, ar_r, rs_s, rs_r,
):
    rows, cols = tok.shape
    seqs, heads, hd = st.shape[1], st.shape[2], st.shape[3]
    width = wq.shape[2]
    pairs = seqs * heads
    features = cols * dp
    me_tp = lax.axis_index("tp")
    me_dp = lax.axis_index("dp")

    def remote(src, dst, send, recv, axis, peer):
        return pltpu.make_async_remote_copy(
            src_ref=src, dst_ref=dst, send_sem=send, recv_sem=recv,
            device_id={axis: peer}, device_id_type=MESH,
        )

    weights = (wq, wf, wv, wg)

    def load_w(l, i):
        return pltpu.make_async_copy(weights[i].at[l], w_v.at[l, i], w_sem.at[l, i])

    def load_wo(l):
        return pltpu.make_async_copy(wo.at[l], wo_v.at[l], wo_sem.at[l])

    def load_s(l):
        return pltpu.make_async_copy(st.at[l], s_v.at[l], s_sem.at[l])

    def store_s(l):
        return pltpu.make_async_copy(s_v.at[l], ns.at[l], o_sem.at[l])

    for l in range(2):
        for i in range(4):
            load_w(l, i).start()
        load_s(l).start()
        load_wo(l).start()

    barrier = pltpu.get_barrier_semaphore()

    def greet_tp(d):
        pl.semaphore_signal(
            barrier, inc=1, device_id={"tp": lax.rem(me_tp + d, tp)}, device_id_type=MESH
        )

    def greet_dp(d):
        pl.semaphore_signal(
            barrier, inc=1, device_id={"dp": lax.rem(me_dp + d, dp)}, device_id_type=MESH
        )

    each(tp, greet_tp)
    each(dp, greet_dp)
    pl.semaphore_wait(barrier, tp + dp - 2)

    def xg_copy(d):
        return remote(tok, xg.at[me_tp], xg_s.at[d], xg_r.at[me_tp], "tp", lax.rem(me_tp + d, tp))

    each(tp, lambda d: xg_copy(d).start())
    xg[me_tp] = tok[...]

    def xg_wait(d):
        src = lax.rem(me_tp + tp - d, tp)
        remote(tok, xg.at[src], xg_s.at[d], xg_r.at[src], "tp", src).wait_recv()

    each(tp, xg_wait)
    for j in range(tp):
        hf[j * rows:(j + 1) * rows, :] = xg[j].astype(F32)

    for l in range(2):
        h = hf[...]
        sq2[...] = jnp.broadcast_to(
            jnp.sum(h * h, axis=1, keepdims=True), (h.shape[0], LANES)
        )
        for j in range(dp):
            sqs[l, j] = sq2[j * seqs:(j + 1) * seqs, :]

        def sq_copy(d):
            peer = lax.rem(me_dp + d, dp)
            return remote(
                sqs.at[l, peer], sqr.at[l, me_dp], sq_s.at[l, d], sq_r.at[l, me_dp], "dp", peer
            )

        each(dp, lambda d: sq_copy(d).start())
        scaled = (h * gain[l:l + 1, :]).astype(BF16)

        def p_copy(i, d):
            peer = lax.rem(me_dp + d, dp)
            return remote(
                ps.at[l, i, peer], pr.at[l, i, me_dp], p_s.at[l, i, d], p_r.at[l, i, me_dp],
                "dp", peer,
            )

        for i in range(4):
            load_w(l, i).wait()
            pf[i] = jnp.dot(scaled, w_v[l, i], preferred_element_type=F32)
            for j in range(dp):
                ps[l, i, j] = pf[i, j * seqs:(j + 1) * seqs, :].astype(BF16)
            each(dp, lambda d: p_copy(i, d).start())

        def sq_wait(d):
            src = lax.rem(me_dp + dp - d, dp)
            remote(
                sqs.at[l, src], sqr.at[l, src], sq_s.at[l, d], sq_r.at[l, src], "dp", src
            ).wait_recv()

        sqr[l, me_dp] = sqs[l, me_dp]
        each(dp, sq_wait)
        total = sqr[l, 0]
        for j in range(1, dp):
            total = total + sqr[l, j]
        factor = lax.rsqrt(total / features + 1e-06)

        load_s(l).wait()
        proj = []
        for i in range(4):

            def p_wait(d):
                src = lax.rem(me_dp + dp - d, dp)
                remote(
                    ps.at[l, i, src], pr.at[l, i, src], p_s.at[l, i, d], p_r.at[l, i, src],
                    "dp", src,
                ).wait_recv()

            pr[l, i, me_dp] = ps[l, i, me_dp]
            each(dp, p_wait)
            acc = pr[l, i, 0].astype(F32)
            for j in range(1, dp):
                acc = acc + pr[l, i, j].astype(F32)
            proj.append(acc)

        values, dots, gates = [], [], []
        for k in range(heads):
            lanes = slice(k * hd, (k + 1) * hd)
            query, forget_pre, value, gate_pre = (proj[i][:, lanes] * factor for i in range(4))
            bound = bound_ref[l:l + 1, lanes]
            forget = bound + (1.0 - bound) * jax.nn.sigmoid(forget_pre)
            keyvec = (1.0 - bound) * jax.nn.sigmoid(-forget_pre)
            tr_a[k * seqs:(k + 1) * seqs, :] = forget * query
            tr_b[k * seqs:(k + 1) * seqs, :] = forget
            tr_b[pairs + k * seqs:pairs + (k + 1) * seqs, :] = keyvec
            values.append(value)
            dots.append(jnp.sum(query * keyvec, axis=1, keepdims=True) * value)
            gates.append(jax.nn.sigmoid(gate_pre))
        cols_a = tr_a[...].T
        for k in range(heads):
            for b in range(seqs):
                p = k * seqs + b
                ro[p:p + 1, :] = jnp.sum(cols_a[:, p:p + 1] * s_v[l, b, k], axis=0, keepdims=True)
        for k in range(heads):
            readout = ro[k * seqs:(k + 1) * seqs, :] + dots[k]
            readout = (
                readout
                * lax.rsqrt(jnp.mean(readout * readout, axis=-1, keepdims=True) + 1e-06)
                * head_gain[l:l + 1, :]
            )
            na[l, me_dp, :, k * hd:(k + 1) * hd] = (readout * gates[k]).astype(BF16)

        def n_copy(d):
            peer = lax.rem(me_dp + d, dp)
            return remote(
                na.at[l, me_dp], na.at[l, me_dp], n_s.at[l, d], n_r.at[l, me_dp], "dp", peer
            )

        each(dp, lambda d: n_copy(d).start())

        cols_b = tr_b[...].T
        for k in range(heads):
            for b in range(seqs):
                p = k * seqs + b
                s_v[l, b, k] = (
                    cols_b[:, p:p + 1] * s_v[l, b, k]
                    + cols_b[:, pairs + p:pairs + p + 1] * values[k][b:b + 1, :]
                )
        store_s(l).start()
        load_wo(l).wait()

        def n_wait(d):
            src = lax.rem(me_dp + dp - d, dp)
            remote(
                na.at[l, src], na.at[l, src], n_s.at[l, d], n_r.at[l, src], "dp", src
            ).wait_recv()

        each(dp, n_wait)
        for j in range(dp):
            nf[j * seqs:(j + 1) * seqs, :] = na[l, j].astype(F32)
        mixed = jnp.dot(nf[...].astype(BF16), wo_v[l], preferred_element_type=F32)

        if l == 0:
            ar[me_tp] = mixed.astype(BF16)

            def ar_copy(d):
                return remote(
                    ar.at[me_tp], ar.at[me_tp], ar_s.at[d], ar_r.at[me_tp], "tp",
                    lax.rem(me_tp + d, tp),
                )

            each(tp, lambda d: ar_copy(d).start())

            def ar_wait(d):
                src = lax.rem(me_tp + tp - d, tp)
                remote(
                    ar.at[src], ar.at[src], ar_s.at[d], ar_r.at[src], "tp", src
                ).wait_recv()

            each(tp, ar_wait)
            acc = ar[0].astype(F32)
            for j in range(1, tp):
                acc = acc + ar[j].astype(F32)
            hf[...] = (hf[...] + acc).astype(BF16).astype(F32)
            for j in range(tp):
                h3[j] = hf[j * rows:(j + 1) * rows, :]
        else:
            po[...] = mixed
            for j in range(tp):
                rs[j] = po[j * rows:(j + 1) * rows, :].astype(BF16)

            def rs_copy(d):
                peer = lax.rem(me_tp + d, tp)
                return remote(
                    rs.at[peer], rr.at[me_tp], rs_s.at[d], rs_r.at[me_tp], "tp", peer
                )

            each(tp, lambda d: rs_copy(d).start())
            rr[me_tp] = rs[me_tp]

            def rs_wait(d):
                src = lax.rem(me_tp + tp - d, tp)
                remote(rs.at[src], rr.at[src], rs_s.at[d], rs_r.at[src], "tp", src).wait_recv()

            each(tp, rs_wait)
            acc = rr[0].astype(F32)
            for j in range(1, tp):
                acc = acc + rr[j].astype(F32)
            out[...] = (h3[me_tp] + acc).astype(BF16)
            each(tp, lambda d: rs_copy(d).wait_send())
            each(tp, lambda d: ar_copy(d).wait_send())
        each(dp, lambda d: sq_copy(d).wait_send())
        for i in range(4):
            each(dp, lambda d: p_copy(i, d).wait_send())
        each(dp, lambda d: n_copy(d).wait_send())
    each(tp, lambda d: xg_copy(d).wait_send())
    for l in range(2):
        store_s(l).wait()


def per_device(
    tp, dp,
    tokens, norm_gain, w_query, w_forget, w_value, w_gate, lower_bound, head_gain, w_out, state
):
    rows, cols = tokens.shape
    seqs = state.shape[1]
    heads = state.shape[2]
    width = w_query.shape[2]
    batch = rows * tp
    pad = -(-2 * seqs * heads // LANES) * LANES
    vmem = pl.BlockSpec(memory_space=pltpu.VMEM)
    hbm = pl.BlockSpec(memory_space=pl.ANY)
    dma = pltpu.SemaphoreType.DMA
    return pl.pallas_call(
        functools.partial(kernel, tp, dp),
        name="two_blocks",
        out_shape=(
            jax.ShapeDtypeStruct(tokens.shape, BF16),
            jax.ShapeDtypeStruct(state.shape, F32),
        ),
        in_specs=[vmem, vmem, hbm, hbm, hbm, hbm, vmem, vmem, hbm, hbm],
        out_specs=(vmem, hbm),
        scratch_shapes=[
            pltpu.VMEM((2, 4, cols, width), BF16),
            pltpu.VMEM((2, width, cols), BF16),
            pltpu.VMEM(state.shape, F32),
            pltpu.VMEM((tp, rows, cols), BF16),
            pltpu.VMEM((batch, cols), F32),
            pltpu.VMEM((tp, rows, cols), F32),
            pltpu.VMEM((batch, LANES), F32),
            pltpu.VMEM((2, dp, seqs, LANES), F32),
            pltpu.VMEM((2, dp, seqs, LANES), F32),
            pltpu.VMEM((4, batch, width), F32),
            pltpu.VMEM((2, 4, dp, seqs, width), BF16),
            pltpu.VMEM((2, 4, dp, seqs, width), BF16),
            pltpu.VMEM((pad, LANES), F32),
            pltpu.VMEM((pad, LANES), F32),
            pltpu.VMEM((max(8, seqs * heads), LANES), F32),
            pltpu.VMEM((2, dp, seqs, width), BF16),
            pltpu.VMEM((batch, width), F32),
            pltpu.VMEM((batch, cols), F32),
            pltpu.VMEM((tp, batch, cols), BF16),
            pltpu.VMEM((tp, rows, cols), BF16),
            pltpu.VMEM((tp, rows, cols), BF16),
            dma((2, 4)), dma((2,)), dma((2,)), dma((2,)),
            dma((tp,)), dma((tp,)),
            dma((2, dp)), dma((2, dp)),
            dma((2, 4, dp)), dma((2, 4, dp)),
            dma((2, dp)), dma((2, dp)),
            dma((tp,)), dma((tp,)), dma((tp,)), dma((tp,)),
        ],
        compiler_params=pltpu.CompilerParams(
            collective_id=0, has_side_effects=True, vmem_limit_bytes=60 * 1024 * 1024
        ),
    )(tokens, norm_gain, w_query, w_forget, w_value, w_gate, lower_bound, head_gain, w_out, state)


def solution(mesh):
    return jax.shard_map(
        functools.partial(per_device, mesh.shape["tp"], mesh.shape["dp"]),
        mesh=mesh,
        in_specs=(
            P(("grp", "tp"), "dp"),
            P(None, "dp"),
            P(None, "dp", "tp"),
            P(None, "dp", "tp"),
            P(None, "dp", "tp"),
            P(None, "dp", "tp"),
            P(None, "tp"),
            P(),
            P(None, "tp", "dp"),
            P(None, ("grp", "dp"), "tp", None, None),
        ),
        out_specs=(P(("grp", "tp"), "dp"), P(None, ("grp", "dp"), "tp", None, None)),
        check_vma=False,
    )
```

```python
import functools

import jax
import jax.numpy as jnp
from jax import lax
from jax.experimental import pallas as pl
from jax.experimental.pallas import tpu as pltpu
from jax.sharding import PartitionSpec as P

MESH = pl.DeviceIdType.MESH
LANES = 128
F32 = jnp.float32
GROUPS = 2
BF16 = jnp.bfloat16


def each(count, body):
    if count <= 8:
        for d in range(1, count):
            body(d)
    else:

        @pl.loop(1, count)
        def _(d):
            body(d)


def kernel(
    tp, dp,
    tok_h, gain_h, wq, wf, wv, wg, bound_h, head_gain_h, wo, st,
    out, s_v,
    tok, gain, bound_ref, head_gain, w_v, wo_v, xg, hf, h3, sq2, sqs, sqr, pf, ps, pr, tr_a, tr_b, ro,
    na, nf, po, ar, rs, rr,
    small_sem, w_sem, wo_sem, s_sem, xg_s, xg_r, sq_s, sq_r, p_s, p_r, n_s, n_r,
    ar_s, ar_r, rs_s, rs_r,
):
    rows, cols = tok.shape
    seqs, heads, hd = st.shape[1], st.shape[2], st.shape[3]
    width = wq.shape[2]
    pairs = seqs * heads
    features = cols * dp
    me_tp = lax.axis_index("tp")
    me_dp = lax.axis_index("dp")

    def remote(src, dst, send, recv, axis, peer):
        return pltpu.make_async_remote_copy(
            src_ref=src, dst_ref=dst, send_sem=send, recv_sem=recv,
            device_id={axis: peer}, device_id_type=MESH,
        )

    weights = (wq, wf, wv, wg)

    def load_w(l, i):
        return pltpu.make_async_copy(weights[i].at[l], w_v.at[l, i], w_sem.at[l, i])

    def load_wo(l):
        return pltpu.make_async_copy(wo.at[l], wo_v.at[l], wo_sem.at[l])

    def load_s(l):
        return pltpu.make_async_copy(st.at[l], s_v.at[l], s_sem.at[l])

    smalls = [
        pltpu.make_async_copy(src, dst, small_sem.at[i])
        for i, (src, dst) in enumerate(
            ((tok_h, tok), (gain_h, gain), (bound_h, bound_ref), (head_gain_h, head_gain))
        )
    ]
    smalls[0].start()
    barrier = pltpu.get_barrier_semaphore()

    def greet_tp(d):
        pl.semaphore_signal(
            barrier, inc=1, device_id={"tp": lax.rem(me_tp + d, tp)}, device_id_type=MESH
        )

    def greet_dp(d):
        pl.semaphore_signal(
            barrier, inc=1, device_id={"dp": lax.rem(me_dp + d, dp)}, device_id_type=MESH
        )

    each(tp, greet_tp)
    each(dp, greet_dp)
    for copy in smalls[1:]:
        copy.start()
    for l in range(2):
        for i in range(4):
            load_w(l, i).start()
        load_s(l).start()
        load_wo(l).start()
    smalls[0].wait()
    pl.semaphore_wait(barrier, tp + dp - 2)

    def xg_copy(d):
        return remote(tok, xg.at[me_tp], xg_s.at[d], xg_r.at[me_tp], "tp", lax.rem(me_tp + d, tp))

    each(tp, lambda d: xg_copy(d).start())
    xg[me_tp] = tok[...]

    def xg_wait(d):
        src = lax.rem(me_tp + tp - d, tp)
        remote(tok, xg.at[src], xg_s.at[d], xg_r.at[src], "tp", src).wait_recv()

    each(tp, xg_wait)
    for j in range(tp):
        hf[j * rows:(j + 1) * rows, :] = xg[j].astype(F32)

    for copy in smalls[1:]:
        copy.wait()
    for l in range(2):
        h = hf[...]
        sq2[...] = jnp.broadcast_to(
            jnp.sum(h * h, axis=1, keepdims=True), (h.shape[0], LANES)
        )
        for j in range(dp):
            sqs[l, j] = sq2[j * seqs:(j + 1) * seqs, :]

        def sq_copy(d):
            peer = lax.rem(me_dp + d, dp)
            return remote(
                sqs.at[l, peer], sqr.at[l, me_dp], sq_s.at[l, d], sq_r.at[l, me_dp], "dp", peer
            )

        each(dp, lambda d: sq_copy(d).start())
        scaled = (h * gain[l:l + 1, :]).astype(BF16)

        def p_copy(i, d):
            peer = lax.rem(me_dp + d, dp)
            return remote(
                ps.at[l, i, peer], pr.at[l, i, me_dp], p_s.at[l, i, d], p_r.at[l, i, me_dp],
                "dp", peer,
            )

        per = 4 // GROUPS
        for i in range(4):
            load_w(l, i).wait()
            pf[i] = jnp.dot(scaled, w_v[l, i], preferred_element_type=F32)
            part = slice(i % per * width, (i % per + 1) * width)
            for j in range(dp):
                ps[l, i // per, j, :, part] = pf[i, j * seqs:(j + 1) * seqs, :].astype(BF16)
            if i % per == per - 1:
                each(dp, lambda d: p_copy(i // per, d).start())

        def sq_wait(d):
            src = lax.rem(me_dp + dp - d, dp)
            remote(
                sqs.at[l, src], sqr.at[l, src], sq_s.at[l, d], sq_r.at[l, src], "dp", src
            ).wait_recv()

        sqr[l, me_dp] = sqs[l, me_dp]
        each(dp, sq_wait)
        total = sqr[l, 0]
        for j in range(1, dp):
            total = total + sqr[l, j]
        factor = lax.rsqrt(total / features + 1e-06)

        load_s(l).wait()
        proj = []
        for i in range(GROUPS):

            def p_wait(d):
                src = lax.rem(me_dp + dp - d, dp)
                remote(
                    ps.at[l, i, src], pr.at[l, i, src], p_s.at[l, i, d], p_r.at[l, i, src],
                    "dp", src,
                ).wait_recv()

            pr[l, i, me_dp] = ps[l, i, me_dp]
            each(dp, p_wait)
            acc = pr[l, i, 0].astype(F32)
            for j in range(1, dp):
                acc = acc + pr[l, i, j].astype(F32)
            proj.extend(acc[:, g * width:(g + 1) * width] for g in range(per))

        values, dots, gates = [], [], []
        for k in range(heads):
            lanes = slice(k * hd, (k + 1) * hd)
            query, forget_pre, value, gate_pre = (proj[i][:, lanes] * factor for i in range(4))
            bound = bound_ref[l:l + 1, lanes]
            forget = bound + (1.0 - bound) * jax.nn.sigmoid(forget_pre)
            keyvec = (1.0 - bound) * jax.nn.sigmoid(-forget_pre)
            tr_a[k * seqs:(k + 1) * seqs, :] = forget * query
            tr_b[k * seqs:(k + 1) * seqs, :] = forget
            tr_b[pairs + k * seqs:pairs + (k + 1) * seqs, :] = keyvec
            values.append(value)
            dots.append(jnp.sum(query * keyvec, axis=1, keepdims=True) * value)
            gates.append(jax.nn.sigmoid(gate_pre))
        cols_a = tr_a[...].T
        for k in range(heads):
            for b in range(seqs):
                p = k * seqs + b
                ro[p:p + 1, :] = jnp.sum(cols_a[:, p:p + 1] * s_v[l, b, k], axis=0, keepdims=True)
        for k in range(heads):
            readout = ro[k * seqs:(k + 1) * seqs, :] + dots[k]
            readout = (
                readout
                * lax.rsqrt(jnp.mean(readout * readout, axis=-1, keepdims=True) + 1e-06)
                * head_gain[l:l + 1, :]
            )
            na[l, me_dp, :, k * hd:(k + 1) * hd] = (readout * gates[k]).astype(BF16)

        def n_copy(d):
            peer = lax.rem(me_dp + d, dp)
            return remote(
                na.at[l, me_dp], na.at[l, me_dp], n_s.at[l, d], n_r.at[l, me_dp], "dp", peer
            )

        each(dp, lambda d: n_copy(d).start())

        cols_b = tr_b[...].T
        for k in range(heads):
            for b in range(seqs):
                p = k * seqs + b
                s_v[l, b, k] = (
                    cols_b[:, p:p + 1] * s_v[l, b, k]
                    + cols_b[:, pairs + p:pairs + p + 1] * values[k][b:b + 1, :]
                )
        load_wo(l).wait()

        def n_wait(d):
            src = lax.rem(me_dp + dp - d, dp)
            remote(
                na.at[l, src], na.at[l, src], n_s.at[l, d], n_r.at[l, src], "dp", src
            ).wait_recv()

        each(dp, n_wait)
        for j in range(dp):
            nf[j * seqs:(j + 1) * seqs, :] = na[l, j].astype(F32)
        mixed = jnp.dot(nf[...].astype(BF16), wo_v[l], preferred_element_type=F32)

        if l == 0:
            ar[me_tp] = mixed.astype(BF16)

            def ar_copy(d):
                return remote(
                    ar.at[me_tp], ar.at[me_tp], ar_s.at[d], ar_r.at[me_tp], "tp",
                    lax.rem(me_tp + d, tp),
                )

            each(tp, lambda d: ar_copy(d).start())

            def ar_wait(d):
                src = lax.rem(me_tp + tp - d, tp)
                remote(
                    ar.at[src], ar.at[src], ar_s.at[d], ar_r.at[src], "tp", src
                ).wait_recv()

            each(tp, ar_wait)
            acc = ar[0].astype(F32)
            for j in range(1, tp):
                acc = acc + ar[j].astype(F32)
            hf[...] = (hf[...] + acc).astype(BF16).astype(F32)
            for j in range(tp):
                h3[j] = hf[j * rows:(j + 1) * rows, :]
        else:
            po[...] = mixed
            for j in range(tp):
                rs[j] = po[j * rows:(j + 1) * rows, :].astype(BF16)

            def rs_copy(d):
                peer = lax.rem(me_tp + d, tp)
                return remote(
                    rs.at[peer], rr.at[me_tp], rs_s.at[d], rs_r.at[me_tp], "tp", peer
                )

            each(tp, lambda d: rs_copy(d).start())
            rr[me_tp] = rs[me_tp]

            def rs_wait(d):
                src = lax.rem(me_tp + tp - d, tp)
                remote(rs.at[src], rr.at[src], rs_s.at[d], rs_r.at[src], "tp", src).wait_recv()

            each(tp, rs_wait)
            acc = rr[0].astype(F32)
            for j in range(1, tp):
                acc = acc + rr[j].astype(F32)
            out[...] = (h3[me_tp] + acc).astype(BF16)
            each(tp, lambda d: rs_copy(d).wait_send())
            each(tp, lambda d: ar_copy(d).wait_send())
        each(dp, lambda d: sq_copy(d).wait_send())
        for i in range(GROUPS):
            each(dp, lambda d: p_copy(i, d).wait_send())
        each(dp, lambda d: n_copy(d).wait_send())
    each(tp, lambda d: xg_copy(d).wait_send())


def per_device(
    tp, dp,
    tokens, norm_gain, w_query, w_forget, w_value, w_gate, lower_bound, head_gain, w_out, state
):
    rows, cols = tokens.shape
    seqs = state.shape[1]
    heads = state.shape[2]
    width = w_query.shape[2]
    batch = rows * tp
    pad = -(-2 * seqs * heads // LANES) * LANES
    vmem = pl.BlockSpec(memory_space=pltpu.VMEM)
    hbm = pl.BlockSpec(memory_space=pltpu.HBM)
    dma = pltpu.SemaphoreType.DMA
    return pl.pallas_call(
        functools.partial(kernel, tp, dp),
        name="two_blocks",
        out_shape=(
            jax.ShapeDtypeStruct(tokens.shape, BF16),
            jax.ShapeDtypeStruct(state.shape, F32),
        ),
        in_specs=[hbm] * 10,
        out_specs=(vmem, vmem),
        scratch_shapes=[
            pltpu.VMEM(tokens.shape, BF16),
            pltpu.VMEM(norm_gain.shape, F32),
            pltpu.VMEM(lower_bound.shape, F32),
            pltpu.VMEM(head_gain.shape, F32),
            pltpu.VMEM((2, 4, cols, width), BF16),
            pltpu.VMEM((2, width, cols), BF16),
            pltpu.VMEM((tp, rows, cols), BF16),
            pltpu.VMEM((batch, cols), F32),
            pltpu.VMEM((tp, rows, cols), F32),
            pltpu.VMEM((batch, LANES), F32),
            pltpu.VMEM((2, dp, seqs, LANES), F32),
            pltpu.VMEM((2, dp, seqs, LANES), F32),
            pltpu.VMEM((4, batch, width), F32),
            pltpu.VMEM((2, GROUPS, dp, seqs, 4 // GROUPS * width), BF16),
            pltpu.VMEM((2, GROUPS, dp, seqs, 4 // GROUPS * width), BF16),
            pltpu.VMEM((pad, LANES), F32),
            pltpu.VMEM((pad, LANES), F32),
            pltpu.VMEM((max(8, seqs * heads), LANES), F32),
            pltpu.VMEM((2, dp, seqs, width), BF16),
            pltpu.VMEM((batch, width), F32),
            pltpu.VMEM((batch, cols), F32),
            pltpu.VMEM((tp, batch, cols), BF16),
            pltpu.VMEM((tp, rows, cols), BF16),
            pltpu.VMEM((tp, rows, cols), BF16),
            dma((4,)), dma((2, 4)), dma((2,)), dma((2,)),
            dma((tp,)), dma((tp,)),
            dma((2, dp)), dma((2, dp)),
            dma((2, GROUPS, dp)), dma((2, GROUPS, dp)),
            dma((2, dp)), dma((2, dp)),
            dma((tp,)), dma((tp,)), dma((tp,)), dma((tp,)),
        ],
        compiler_params=pltpu.CompilerParams(
            collective_id=0, has_side_effects=True, vmem_limit_bytes=32 * 1024 * 1024
        ),
    )(*(
        pltpu.with_memory_space_constraint(array, pltpu.HBM)
        for array in (
            tokens, norm_gain, w_query, w_forget, w_value, w_gate, lower_bound, head_gain, w_out,
            state,
        )
    ))


def solution(mesh):
    return jax.shard_map(
        functools.partial(per_device, mesh.shape["tp"], mesh.shape["dp"]),
        mesh=mesh,
        in_specs=(
            P(("grp", "tp"), "dp"),
            P(None, "dp"),
            P(None, "dp", "tp"),
            P(None, "dp", "tp"),
            P(None, "dp", "tp"),
            P(None, "dp", "tp"),
            P(None, "tp"),
            P(),
            P(None, "tp", "dp"),
            P(None, ("grp", "dp"), "tp", None, None),
        ),
        out_specs=(P(("grp", "tp"), "dp"), P(None, ("grp", "dp"), "tp", None, None)),
        check_vma=False,
    )
```

```python
import functools

import jax
import jax.numpy as jnp
from jax import lax
from jax.experimental import pallas as pl
from jax.experimental.pallas import tpu as pltpu
from jax.sharding import PartitionSpec as P

MESH = pl.DeviceIdType.MESH
LANES = 128
F32 = jnp.float32
GROUPS = 2
BF16 = jnp.bfloat16


def each(count, body):
    if count <= 8:
        for d in range(1, count):
            body(d)
    else:

        @pl.loop(1, count)
        def _(d):
            body(d)


def kernel(
    tp, dp,
    tok_h, gain_h, wq, wf, wv, wg, bound_h, head_gain_h, wo, st,
    out, s_v,
    tok, gain, bound_ref, head_gain, w_v, wo_v, xg, hf, h3, sq2, sqs, sqr, pf, ps, pr, tr_a, tr_b, ro,
    na, nf, po, ar, rs, rr,
    small_sem, w_sem, wo_sem, s_sem, xg_s, xg_r, sq_s, sq_r, p_s, p_r, n_s, n_r,
    ar_s, ar_r, rs_s, rs_r,
):
    rows, cols = tok.shape
    seqs, heads, hd = st.shape[1], st.shape[2], st.shape[3]
    width = wq.shape[2]
    pairs = seqs * heads
    features = cols * dp
    me_tp = lax.axis_index("tp")
    me_dp = lax.axis_index("dp")

    def remote(src, dst, send, recv, axis, peer):
        return pltpu.make_async_remote_copy(
            src_ref=src, dst_ref=dst, send_sem=send, recv_sem=recv,
            device_id={axis: peer}, device_id_type=MESH,
        )

    def far(k):
        above = tp - me_tp
        return jnp.where(k < above, tp - k, k - above)

    weights = (wq, wf, wv, wg)

    def load_w(l, i):
        return pltpu.make_async_copy(weights[i].at[l], w_v.at[l, i], w_sem.at[l, i])

    def load_wo(l):
        return pltpu.make_async_copy(wo.at[l], wo_v.at[l], wo_sem.at[l])

    def load_s(l):
        return pltpu.make_async_copy(st.at[l], s_v.at[l], s_sem.at[l])

    smalls = [
        pltpu.make_async_copy(src, dst, small_sem.at[i])
        for i, (src, dst) in enumerate(
            ((tok_h, tok), (gain_h, gain), (bound_h, bound_ref), (head_gain_h, head_gain))
        )
    ]
    smalls[0].start()
    barrier = pltpu.get_barrier_semaphore()

    def greet_tp(d):
        pl.semaphore_signal(
            barrier, inc=1, device_id={"tp": lax.rem(me_tp + d, tp)}, device_id_type=MESH
        )

    def greet_dp(d):
        pl.semaphore_signal(
            barrier, inc=1, device_id={"dp": lax.rem(me_dp + d, dp)}, device_id_type=MESH
        )

    each(tp, greet_tp)
    each(dp, greet_dp)
    for copy in smalls[1:]:
        copy.start()
    for l in range(2):
        for i in range(4):
            load_w(l, i).start()
        load_s(l).start()
        load_wo(l).start()
    smalls[0].wait()
    pl.semaphore_wait(barrier, tp + dp - 2)

    def xg_copy(d):
        return remote(tok, xg.at[me_tp], xg_s.at[d], xg_r.at[me_tp], "tp", far(d))

    each(tp, lambda d: xg_copy(d).start())
    xg[me_tp] = tok[...]

    def xg_wait(d):
        src = lax.rem(me_tp + tp - d, tp)
        remote(tok, xg.at[src], xg_s.at[d], xg_r.at[src], "tp", src).wait_recv()

    each(tp, xg_wait)
    for j in range(tp):
        hf[j * rows:(j + 1) * rows, :] = xg[j].astype(F32)

    for copy in smalls[1:]:
        copy.wait()
    for l in range(2):
        h = hf[...]
        sq2[...] = jnp.broadcast_to(
            jnp.sum(h * h, axis=1, keepdims=True), (h.shape[0], LANES)
        )
        for j in range(dp):
            sqs[l, j] = sq2[j * seqs:(j + 1) * seqs, :]

        def sq_copy(d):
            peer = lax.rem(me_dp + d, dp)
            return remote(
                sqs.at[l, peer], sqr.at[l, me_dp], sq_s.at[l, d], sq_r.at[l, me_dp], "dp", peer
            )

        each(dp, lambda d: sq_copy(d).start())
        scaled = (h * gain[l:l + 1, :]).astype(BF16)

        def p_copy(i, d):
            peer = lax.rem(me_dp + d, dp)
            return remote(
                ps.at[l, i, peer], pr.at[l, i, me_dp], p_s.at[l, i, d], p_r.at[l, i, me_dp],
                "dp", peer,
            )

        per = 4 // GROUPS
        for i in range(4):
            load_w(l, i).wait()
            pf[i] = jnp.dot(scaled, w_v[l, i], preferred_element_type=F32)
            part = slice(i % per * width, (i % per + 1) * width)
            for j in range(dp):
                ps[l, i // per, j, :, part] = pf[i, j * seqs:(j + 1) * seqs, :].astype(BF16)
            if i % per == per - 1:
                each(dp, lambda d: p_copy(i // per, d).start())

        def sq_wait(d):
            src = lax.rem(me_dp + dp - d, dp)
            remote(
                sqs.at[l, src], sqr.at[l, src], sq_s.at[l, d], sq_r.at[l, src], "dp", src
            ).wait_recv()

        sqr[l, me_dp] = sqs[l, me_dp]
        each(dp, sq_wait)
        total = sqr[l, 0]
        for j in range(1, dp):
            total = total + sqr[l, j]
        factor = lax.rsqrt(total / features + 1e-06)

        load_s(l).wait()
        proj = []
        for i in range(GROUPS):

            def p_wait(d):
                src = lax.rem(me_dp + dp - d, dp)
                remote(
                    ps.at[l, i, src], pr.at[l, i, src], p_s.at[l, i, d], p_r.at[l, i, src],
                    "dp", src,
                ).wait_recv()

            pr[l, i, me_dp] = ps[l, i, me_dp]
            each(dp, p_wait)
            acc = pr[l, i, 0].astype(F32)
            for j in range(1, dp):
                acc = acc + pr[l, i, j].astype(F32)
            proj.extend(acc[:, g * width:(g + 1) * width] for g in range(per))

        values, dots, gates = [], [], []
        for k in range(heads):
            lanes = slice(k * hd, (k + 1) * hd)
            query, forget_pre, value, gate_pre = (proj[i][:, lanes] * factor for i in range(4))
            bound = bound_ref[l:l + 1, lanes]
            forget = bound + (1.0 - bound) * jax.nn.sigmoid(forget_pre)
            keyvec = (1.0 - bound) * jax.nn.sigmoid(-forget_pre)
            tr_a[k * seqs:(k + 1) * seqs, :] = forget * query
            tr_b[k * seqs:(k + 1) * seqs, :] = forget
            tr_b[pairs + k * seqs:pairs + (k + 1) * seqs, :] = keyvec
            values.append(value)
            dots.append(jnp.sum(query * keyvec, axis=1, keepdims=True) * value)
            gates.append(jax.nn.sigmoid(gate_pre))
        cols_a = tr_a[...].T
        for k in range(heads):
            for b in range(seqs):
                p = k * seqs + b
                ro[p:p + 1, :] = jnp.sum(cols_a[:, p:p + 1] * s_v[l, b, k], axis=0, keepdims=True)
        for k in range(heads):
            readout = ro[k * seqs:(k + 1) * seqs, :] + dots[k]
            readout = (
                readout
                * lax.rsqrt(jnp.mean(readout * readout, axis=-1, keepdims=True) + 1e-06)
                * head_gain[l:l + 1, :]
            )
            na[l, me_dp, :, k * hd:(k + 1) * hd] = (readout * gates[k]).astype(BF16)

        def n_copy(d):
            peer = lax.rem(me_dp + d, dp)
            return remote(
                na.at[l, me_dp], na.at[l, me_dp], n_s.at[l, d], n_r.at[l, me_dp], "dp", peer
            )

        each(dp, lambda d: n_copy(d).start())

        cols_b = tr_b[...].T
        for k in range(heads):
            for b in range(seqs):
                p = k * seqs + b
                s_v[l, b, k] = (
                    cols_b[:, p:p + 1] * s_v[l, b, k]
                    + cols_b[:, pairs + p:pairs + p + 1] * values[k][b:b + 1, :]
                )
        load_wo(l).wait()

        def n_wait(d):
            src = lax.rem(me_dp + dp - d, dp)
            remote(
                na.at[l, src], na.at[l, src], n_s.at[l, d], n_r.at[l, src], "dp", src
            ).wait_recv()

        each(dp, n_wait)
        for j in range(dp):
            nf[j * seqs:(j + 1) * seqs, :] = na[l, j].astype(F32)
        mixed = jnp.dot(nf[...].astype(BF16), wo_v[l], preferred_element_type=F32)

        if l == 0:
            ar[me_tp] = mixed.astype(BF16)

            def ar_copy(d):
                return remote(
                    ar.at[me_tp], ar.at[me_tp], ar_s.at[d], ar_r.at[me_tp], "tp",
                    far(d),
                )

            each(tp, lambda d: ar_copy(d).start())

            def ar_wait(d):
                src = lax.rem(me_tp + tp - d, tp)
                remote(
                    ar.at[src], ar.at[src], ar_s.at[d], ar_r.at[src], "tp", src
                ).wait_recv()

            each(tp, ar_wait)
            acc = ar[0].astype(F32)
            for j in range(1, tp):
                acc = acc + ar[j].astype(F32)
            hf[...] = (hf[...] + acc).astype(BF16).astype(F32)
            for j in range(tp):
                h3[j] = hf[j * rows:(j + 1) * rows, :]
        else:
            po[...] = mixed
            for j in range(tp):
                rs[j] = po[j * rows:(j + 1) * rows, :].astype(BF16)

            def rs_copy(d):
                peer = far(d)
                return remote(
                    rs.at[peer], rr.at[me_tp], rs_s.at[d], rs_r.at[me_tp], "tp", peer
                )

            each(tp, lambda d: rs_copy(d).start())
            rr[me_tp] = rs[me_tp]

            def rs_wait(d):
                src = lax.rem(me_tp + tp - d, tp)
                remote(rs.at[src], rr.at[src], rs_s.at[d], rs_r.at[src], "tp", src).wait_recv()

            each(tp, rs_wait)
            acc = rr[0].astype(F32)
            for j in range(1, tp):
                acc = acc + rr[j].astype(F32)
            out[...] = (h3[me_tp] + acc).astype(BF16)
            each(tp, lambda d: rs_copy(d).wait_send())
            each(tp, lambda d: ar_copy(d).wait_send())
        each(dp, lambda d: sq_copy(d).wait_send())
        for i in range(GROUPS):
            each(dp, lambda d: p_copy(i, d).wait_send())
        each(dp, lambda d: n_copy(d).wait_send())
    each(tp, lambda d: xg_copy(d).wait_send())


def per_device(
    tp, dp,
    tokens, norm_gain, w_query, w_forget, w_value, w_gate, lower_bound, head_gain, w_out, state
):
    rows, cols = tokens.shape
    seqs = state.shape[1]
    heads = state.shape[2]
    width = w_query.shape[2]
    batch = rows * tp
    pad = -(-2 * seqs * heads // LANES) * LANES
    vmem = pl.BlockSpec(memory_space=pltpu.VMEM)
    hbm = pl.BlockSpec(memory_space=pltpu.HBM)
    dma = pltpu.SemaphoreType.DMA
    return pl.pallas_call(
        functools.partial(kernel, tp, dp),
        name="two_blocks",
        out_shape=(
            jax.ShapeDtypeStruct(tokens.shape, BF16),
            jax.ShapeDtypeStruct(state.shape, F32),
        ),
        in_specs=[hbm] * 10,
        out_specs=(vmem, vmem),
        scratch_shapes=[
            pltpu.VMEM(tokens.shape, BF16),
            pltpu.VMEM(norm_gain.shape, F32),
            pltpu.VMEM(lower_bound.shape, F32),
            pltpu.VMEM(head_gain.shape, F32),
            pltpu.VMEM((2, 4, cols, width), BF16),
            pltpu.VMEM((2, width, cols), BF16),
            pltpu.VMEM((tp, rows, cols), BF16),
            pltpu.VMEM((batch, cols), F32),
            pltpu.VMEM((tp, rows, cols), F32),
            pltpu.VMEM((batch, LANES), F32),
            pltpu.VMEM((2, dp, seqs, LANES), F32),
            pltpu.VMEM((2, dp, seqs, LANES), F32),
            pltpu.VMEM((4, batch, width), F32),
            pltpu.VMEM((2, GROUPS, dp, seqs, 4 // GROUPS * width), BF16),
            pltpu.VMEM((2, GROUPS, dp, seqs, 4 // GROUPS * width), BF16),
            pltpu.VMEM((pad, LANES), F32),
            pltpu.VMEM((pad, LANES), F32),
            pltpu.VMEM((max(8, seqs * heads), LANES), F32),
            pltpu.VMEM((2, dp, seqs, width), BF16),
            pltpu.VMEM((batch, width), F32),
            pltpu.VMEM((batch, cols), F32),
            pltpu.VMEM((tp, batch, cols), BF16),
            pltpu.VMEM((tp, rows, cols), BF16),
            pltpu.VMEM((tp, rows, cols), BF16),
            dma((4,)), dma((2, 4)), dma((2,)), dma((2,)),
            dma((tp,)), dma((tp,)),
            dma((2, dp)), dma((2, dp)),
            dma((2, GROUPS, dp)), dma((2, GROUPS, dp)),
            dma((2, dp)), dma((2, dp)),
            dma((tp,)), dma((tp,)), dma((tp,)), dma((tp,)),
        ],
        compiler_params=pltpu.CompilerParams(
            collective_id=0, has_side_effects=True, vmem_limit_bytes=32 * 1024 * 1024
        ),
    )(*(
        pltpu.with_memory_space_constraint(array, pltpu.HBM)
        for array in (
            tokens, norm_gain, w_query, w_forget, w_value, w_gate, lower_bound, head_gain, w_out,
            state,
        )
    ))


def solution(mesh):
    return jax.shard_map(
        functools.partial(per_device, mesh.shape["tp"], mesh.shape["dp"]),
        mesh=mesh,
        in_specs=(
            P(("grp", "tp"), "dp"),
            P(None, "dp"),
            P(None, "dp", "tp"),
            P(None, "dp", "tp"),
            P(None, "dp", "tp"),
            P(None, "dp", "tp"),
            P(None, "tp"),
            P(),
            P(None, "tp", "dp"),
            P(None, ("grp", "dp"), "tp", None, None),
        ),
        out_specs=(P(("grp", "tp"), "dp"), P(None, ("grp", "dp"), "tp", None, None)),
        check_vma=False,
    )
```

```python
import functools

import jax
import jax.numpy as jnp
from jax import lax
from jax.experimental import pallas as pl
from jax.experimental.pallas import tpu as pltpu
from jax.sharding import PartitionSpec as P

MESH = pl.DeviceIdType.MESH
LANES = 128
F32 = jnp.float32
GROUPS = 2
BF16 = jnp.bfloat16


def each(count, body):
    if count <= 8:
        for d in range(1, count):
            body(d)
    else:

        @pl.loop(1, count)
        def _(d):
            body(d)


def kernel(
    tp, dp,
    tok_h, gain_h, wq, wf, wv, wg, bound_h, head_gain_h, wo, st,
    out, s_v,
    tok, gain, bound_ref, head_gain, w_v, wo_v, xg, hf, h3, sq2, sqs, sqr, pf, ps, pr, tr_a, tr_b, ro,
    na, nf, po, ar, rs, rr,
    small_sem, w_sem, wo_sem, s_sem, xg_s, xg_r, sq_s, sq_r, p_s, p_r, n_s, n_r,
    ar_s, ar_r, rs_s, rs_r,
):
    rows, cols = tok.shape
    seqs, heads, hd = st.shape[1], st.shape[2], st.shape[3]
    width = wq.shape[2]
    pairs = seqs * heads
    chunks = ar.shape[0]
    features = cols * dp
    me_tp = lax.axis_index("tp")
    me_dp = lax.axis_index("dp")

    def remote(src, dst, send, recv, axis, peer):
        return pltpu.make_async_remote_copy(
            src_ref=src, dst_ref=dst, send_sem=send, recv_sem=recv,
            device_id={axis: peer}, device_id_type=MESH,
        )

    def far(k):
        above = tp - me_tp
        return jnp.where(k < above, tp - k, k - above)

    weights = (wq, wf, wv, wg)

    def load_w(l, i):
        return pltpu.make_async_copy(weights[i].at[l], w_v.at[l, i], w_sem.at[l, i])

    def load_wo(l):
        return pltpu.make_async_copy(wo.at[l], wo_v.at[l], wo_sem.at[l])

    def load_s(l):
        return pltpu.make_async_copy(st.at[l], s_v.at[l], s_sem.at[l])

    smalls = [
        pltpu.make_async_copy(src, dst, small_sem.at[i])
        for i, (src, dst) in enumerate(
            ((tok_h, tok), (gain_h, gain), (bound_h, bound_ref), (head_gain_h, head_gain))
        )
    ]
    smalls[0].start()
    barrier = pltpu.get_barrier_semaphore()

    def greet_tp(d):
        pl.semaphore_signal(
            barrier, inc=1, device_id={"tp": lax.rem(me_tp + d, tp)}, device_id_type=MESH
        )

    def greet_dp(d):
        pl.semaphore_signal(
            barrier, inc=1, device_id={"dp": lax.rem(me_dp + d, dp)}, device_id_type=MESH
        )

    each(tp, greet_tp)
    each(dp, greet_dp)
    for copy in smalls[1:]:
        copy.start()
    for l in range(2):
        for i in range(4):
            load_w(l, i).start()
        load_s(l).start()
        load_wo(l).start()
    smalls[0].wait()
    pl.semaphore_wait(barrier, tp + dp - 2)

    def xg_copy(d):
        return remote(tok, xg.at[me_tp], xg_s.at[d], xg_r.at[me_tp], "tp", far(d))

    each(tp, lambda d: xg_copy(d).start())
    xg[me_tp] = tok[...]

    def xg_wait(d):
        src = lax.rem(me_tp + tp - d, tp)
        remote(tok, xg.at[src], xg_s.at[d], xg_r.at[src], "tp", src).wait_recv()

    each(tp, xg_wait)
    for j in range(tp):
        hf[j * rows:(j + 1) * rows, :] = xg[j].astype(F32)

    for copy in smalls[1:]:
        copy.wait()
    for l in range(2):
        steps = chunks if l else 1
        step = cols // steps
        squares = 0.0
        for c in range(steps):
            at = slice(c * step, (c + 1) * step)
            if l:
                each(tp, lambda d: ar_copy(c, d, True).wait_recv())
                acc = ar[c, 0].astype(F32)
                for j in range(1, tp):
                    acc = acc + ar[c, j].astype(F32)
                hf[:, at] = (hf[:, at] + acc).astype(BF16).astype(F32)
            h = hf[:, at]
            squares = squares + jnp.sum(h * h, axis=1, keepdims=True)
            scaled = (h * gain[l:l + 1, at]).astype(BF16)
            if c < steps - 1:
                for i in range(4):
                    if c == 0:
                        load_w(l, i).wait()
                    part = jnp.dot(scaled, w_v[l, i, at, :], preferred_element_type=F32)
                    pf[i] = part if c == 0 else pf[i] + part
        sq2[...] = jnp.broadcast_to(squares, (squares.shape[0], LANES))
        for j in range(dp):
            sqs[l, j] = sq2[j * seqs:(j + 1) * seqs, :]

        def sq_copy(d):
            peer = lax.rem(me_dp + d, dp)
            return remote(
                sqs.at[l, peer], sqr.at[l, me_dp], sq_s.at[l, d], sq_r.at[l, me_dp], "dp", peer
            )

        each(dp, lambda d: sq_copy(d).start())

        def p_copy(i, d):
            peer = lax.rem(me_dp + d, dp)
            return remote(
                ps.at[l, i, peer], pr.at[l, i, me_dp], p_s.at[l, i, d], p_r.at[l, i, me_dp],
                "dp", peer,
            )

        per = 4 // GROUPS
        for i in range(4):
            if steps == 1:
                load_w(l, i).wait()
            rest = jnp.dot(scaled, w_v[l, i, at, :], preferred_element_type=F32)
            pf[i] = rest if steps == 1 else pf[i] + rest
            part = slice(i % per * width, (i % per + 1) * width)
            for j in range(dp):
                ps[l, i // per, j, :, part] = pf[i, j * seqs:(j + 1) * seqs, :].astype(BF16)
            if i % per == per - 1:
                each(dp, lambda d: p_copy(i // per, d).start())

        def sq_wait(d):
            src = lax.rem(me_dp + dp - d, dp)
            remote(
                sqs.at[l, src], sqr.at[l, src], sq_s.at[l, d], sq_r.at[l, src], "dp", src
            ).wait_recv()

        sqr[l, me_dp] = sqs[l, me_dp]
        each(dp, sq_wait)
        total = sqr[l, 0]
        for j in range(1, dp):
            total = total + sqr[l, j]
        factor = lax.rsqrt(total / features + 1e-06)

        load_s(l).wait()
        proj = []
        for i in range(GROUPS):

            def p_wait(d):
                src = lax.rem(me_dp + dp - d, dp)
                remote(
                    ps.at[l, i, src], pr.at[l, i, src], p_s.at[l, i, d], p_r.at[l, i, src],
                    "dp", src,
                ).wait_recv()

            pr[l, i, me_dp] = ps[l, i, me_dp]
            each(dp, p_wait)
            acc = pr[l, i, 0].astype(F32)
            for j in range(1, dp):
                acc = acc + pr[l, i, j].astype(F32)
            proj.extend(acc[:, g * width:(g + 1) * width] for g in range(per))

        values, dots, gates = [], [], []
        for k in range(heads):
            lanes = slice(k * hd, (k + 1) * hd)
            query, forget_pre, value, gate_pre = (proj[i][:, lanes] * factor for i in range(4))
            bound = bound_ref[l:l + 1, lanes]
            forget = bound + (1.0 - bound) * jax.nn.sigmoid(forget_pre)
            keyvec = (1.0 - bound) * jax.nn.sigmoid(-forget_pre)
            tr_a[k * seqs:(k + 1) * seqs, :] = forget * query
            tr_b[k * seqs:(k + 1) * seqs, :] = forget
            tr_b[pairs + k * seqs:pairs + (k + 1) * seqs, :] = keyvec
            values.append(value)
            dots.append(jnp.sum(query * keyvec, axis=1, keepdims=True) * value)
            gates.append(jax.nn.sigmoid(gate_pre))
        cols_a = tr_a[...].T
        for k in range(heads):
            for b in range(seqs):
                p = k * seqs + b
                ro[p:p + 1, :] = jnp.sum(cols_a[:, p:p + 1] * s_v[l, b, k], axis=0, keepdims=True)
        for k in range(heads):
            readout = ro[k * seqs:(k + 1) * seqs, :] + dots[k]
            readout = (
                readout
                * lax.rsqrt(jnp.mean(readout * readout, axis=-1, keepdims=True) + 1e-06)
                * head_gain[l:l + 1, :]
            )
            na[l, me_dp, :, k * hd:(k + 1) * hd] = (readout * gates[k]).astype(BF16)

        def n_copy(d):
            peer = lax.rem(me_dp + d, dp)
            return remote(
                na.at[l, me_dp], na.at[l, me_dp], n_s.at[l, d], n_r.at[l, me_dp], "dp", peer
            )

        each(dp, lambda d: n_copy(d).start())

        cols_b = tr_b[...].T
        for k in range(heads):
            for b in range(seqs):
                p = k * seqs + b
                s_v[l, b, k] = (
                    cols_b[:, p:p + 1] * s_v[l, b, k]
                    + cols_b[:, pairs + p:pairs + p + 1] * values[k][b:b + 1, :]
                )
        load_wo(l).wait()

        def n_wait(d):
            src = lax.rem(me_dp + dp - d, dp)
            remote(
                na.at[l, src], na.at[l, src], n_s.at[l, d], n_r.at[l, src], "dp", src
            ).wait_recv()

        each(dp, n_wait)
        for j in range(dp):
            nf[j * seqs:(j + 1) * seqs, :] = na[l, j].astype(F32)
        gathered = nf[...].astype(BF16)

        if l == 0:

            def ar_copy(c, d, incoming=False):
                src = lax.rem(me_tp + tp - d, tp) if incoming else me_tp
                return remote(
                    ar.at[c, src], ar.at[c, src], ar_s.at[c, d], ar_r.at[c, src], "tp",
                    src if incoming else far(d),
                )

            for c in range(chunks):
                ar[c, me_tp] = jnp.dot(
                    gathered,
                    wo_v[l, :, c * (cols // chunks):(c + 1) * (cols // chunks)],
                    preferred_element_type=F32,
                ).astype(BF16)
                each(tp, lambda d: ar_copy(c, d).start())
        else:
            for j in range(tp):
                h3[j] = hf[j * rows:(j + 1) * rows, :]
            po[...] = jnp.dot(gathered, wo_v[l], preferred_element_type=F32)
            for j in range(tp):
                rs[j] = po[j * rows:(j + 1) * rows, :].astype(BF16)

            def rs_copy(d):
                peer = far(d)
                return remote(
                    rs.at[peer], rr.at[me_tp], rs_s.at[d], rs_r.at[me_tp], "tp", peer
                )

            each(tp, lambda d: rs_copy(d).start())
            rr[me_tp] = rs[me_tp]

            def rs_wait(d):
                src = lax.rem(me_tp + tp - d, tp)
                remote(rs.at[src], rr.at[src], rs_s.at[d], rs_r.at[src], "tp", src).wait_recv()

            each(tp, rs_wait)
            acc = rr[0].astype(F32)
            for j in range(1, tp):
                acc = acc + rr[j].astype(F32)
            out[...] = (h3[me_tp] + acc).astype(BF16)
            each(tp, lambda d: rs_copy(d).wait_send())
            for c in range(chunks):
                each(tp, lambda d: ar_copy(c, d).wait_send())
        each(dp, lambda d: sq_copy(d).wait_send())
        for i in range(GROUPS):
            each(dp, lambda d: p_copy(i, d).wait_send())
        each(dp, lambda d: n_copy(d).wait_send())
    each(tp, lambda d: xg_copy(d).wait_send())


def per_device(
    tp, dp,
    tokens, norm_gain, w_query, w_forget, w_value, w_gate, lower_bound, head_gain, w_out, state
):
    rows, cols = tokens.shape
    seqs = state.shape[1]
    heads = state.shape[2]
    width = w_query.shape[2]
    batch = rows * tp
    chunks = 2 if cols % (2 * LANES) == 0 else 1
    pad = -(-2 * seqs * heads // LANES) * LANES
    vmem = pl.BlockSpec(memory_space=pltpu.VMEM)
    hbm = pl.BlockSpec(memory_space=pltpu.HBM)
    dma = pltpu.SemaphoreType.DMA
    return pl.pallas_call(
        functools.partial(kernel, tp, dp),
        name="two_blocks",
        out_shape=(
            jax.ShapeDtypeStruct(tokens.shape, BF16),
            jax.ShapeDtypeStruct(state.shape, F32),
        ),
        in_specs=[hbm] * 10,
        out_specs=(vmem, vmem),
        scratch_shapes=[
            pltpu.VMEM(tokens.shape, BF16),
            pltpu.VMEM(norm_gain.shape, F32),
            pltpu.VMEM(lower_bound.shape, F32),
            pltpu.VMEM(head_gain.shape, F32),
            pltpu.VMEM((2, 4, cols, width), BF16),
            pltpu.VMEM((2, width, cols), BF16),
            pltpu.VMEM((tp, rows, cols), BF16),
            pltpu.VMEM((batch, cols), F32),
            pltpu.VMEM((tp, rows, cols), F32),
            pltpu.VMEM((batch, LANES), F32),
            pltpu.VMEM((2, dp, seqs, LANES), F32),
            pltpu.VMEM((2, dp, seqs, LANES), F32),
            pltpu.VMEM((4, batch, width), F32),
            pltpu.VMEM((2, GROUPS, dp, seqs, 4 // GROUPS * width), BF16),
            pltpu.VMEM((2, GROUPS, dp, seqs, 4 // GROUPS * width), BF16),
            pltpu.VMEM((pad, LANES), F32),
            pltpu.VMEM((pad, LANES), F32),
            pltpu.VMEM((max(8, seqs * heads), LANES), F32),
            pltpu.VMEM((2, dp, seqs, width), BF16),
            pltpu.VMEM((batch, width), F32),
            pltpu.VMEM((batch, cols), F32),
            pltpu.VMEM((chunks, tp, batch, cols // chunks), BF16),
            pltpu.VMEM((tp, rows, cols), BF16),
            pltpu.VMEM((tp, rows, cols), BF16),
            dma((4,)), dma((2, 4)), dma((2,)), dma((2,)),
            dma((tp,)), dma((tp,)),
            dma((2, dp)), dma((2, dp)),
            dma((2, GROUPS, dp)), dma((2, GROUPS, dp)),
            dma((2, dp)), dma((2, dp)),
            dma((chunks, tp)), dma((chunks, tp)), dma((tp,)), dma((tp,)),
        ],
        compiler_params=pltpu.CompilerParams(
            collective_id=0, has_side_effects=True, vmem_limit_bytes=32 * 1024 * 1024
        ),
    )(*(
        pltpu.with_memory_space_constraint(array, pltpu.HBM)
        for array in (
            tokens, norm_gain, w_query, w_forget, w_value, w_gate, lower_bound, head_gain, w_out,
            state,
        )
    ))


def solution(mesh):
    return jax.shard_map(
        functools.partial(per_device, mesh.shape["tp"], mesh.shape["dp"]),
        mesh=mesh,
        in_specs=(
            P(("grp", "tp"), "dp"),
            P(None, "dp"),
            P(None, "dp", "tp"),
            P(None, "dp", "tp"),
            P(None, "dp", "tp"),
            P(None, "dp", "tp"),
            P(None, "tp"),
            P(),
            P(None, "tp", "dp"),
            P(None, ("grp", "dp"), "tp", None, None),
        ),
        out_specs=(P(("grp", "tp"), "dp"), P(None, ("grp", "dp"), "tp", None, None)),
        check_vma=False,
    )
```
